32 devices in a mesh: sp: 8 (over z, x), tp: 4 (over y, core).
Axes of the slice: x: 2, y: 2, z: 4, core: 2. Of those that a mesh axis runs over, the one named last changes fastest.
Arguments:
- conv_value: bfloat16 [2048, 1024], P('sp', 'tp'), may hold values from -15 to 15
- conv_gate: bfloat16 [2048, 1024], P('sp', 'tp'), may hold values from -8 to 8
- conv_taps: bfloat16 [31, 1024], P(None, 'tp'), may hold values from -1 to 1
- conv_gain: float32 [1024], P('tp'), may hold values from 0.1 to 1.9
- out_weight: bfloat16 [1024, 2048], P('tp'), may hold values from -0.1875 to 0.1875
- residual: bfloat16 [2048, 2048], P('sp'), may hold values from -6 to 6
- route_ids: int32 [2048, 2], P('sp'), may hold values from 0 to 7, all different within a row; in each aligned block of 256 rows (0 to 255, 256 to 511, ...) at most 128 rows name the same one
- route_weight: float32 [2048, 2], P('sp'), may hold values from 0.3 to 1.5
- expert_gate: bfloat16 [8, 2048, 4096], P('sp', None, 'tp'), may hold values from -0.125 to 0.125
- expert_up: bfloat16 [8, 2048, 4096], P('sp', None, 'tp'), may hold values from -0.125 to 0.125
- expert_down: bfloat16 [8, 4096, 2048], P('sp', 'tp'), may hold values from -0.09375 to 0.09375
Outputs:
- layer_out: bfloat16 [2048, 2048], P('sp', 'tp')
The draws below stay inside these ranges and needn't reach their ends.
Inputs may be any that keep to these rules, and one draw needn't show every extreme that they name: `route_ids`: in each aligned block of 256 rows no expert is named by more than 128 rows; some expert is named by exactly 128 rows in some blocks.
All inputs are finite; a program needn't handle non-finite values.
Results may differ from the reference program's by a relative error of at most 0.017.
Values may be sent and summed in bfloat16 or wider, within the bound.
A program may use at most 64 MiB of HBM per device.

```python
import math
from functools import partial
import jax
import jax.numpy as jnp
import numpy as np
from jax import lax

D = 2048
CH = 1024
KW = 31
EXPERT_FF = 4096
TOP_K = 2
TOK_DEV = 256
TOKENS = 2048
EXPERTS = 8
CAP = 128
N_SP = 8
N_TP = 4


def draw_conv_value(key, part):
    spread = jnp.exp(jnp.log(6.0) * jnp.arange(CH, dtype=jnp.float32) / CH)
    sample = jnp.clip(jax.random.normal(key, (TOKENS, CH), jnp.float32), -5.0, 5.0)
    return (0.5 * sample * spread[None, :]).astype(jnp.bfloat16)


def levels(stream_key, dims, cuts, low, largest):
    def one(dim, blocks):
        steps = jax.random.uniform(jax.random.fold_in(jax.random.fold_in(stream_key, 6), dim), (blocks,), jnp.float32, low / len(cuts), largest / len(cuts))
        return jnp.repeat(jnp.exp(steps), dims[dim] // blocks).reshape((-1,) + (1,) * (len(dims) - dim - 1))

    level = one(*cuts[0])
    for cut in cuts[1:]:
        level = level * one(*cut)
    return level


def routed_block(own_key, own, number, rows, amount, top, bound, lean):
    order = jax.random.permutation(own_key, amount)
    crowded, usual = load_shares(amount, rows * top, bound, lean, True), load_shares(amount, rows * top, bound, lean, False)
    places = jnp.arange(amount)

    def named(lengths, turn):
        used = int((lengths > 0).sum())
        fixed = max(1, used // 4)
        moved = fixed + (places - fixed + turn * (used - fixed)) % max(1, amount - fixed)
        return jnp.zeros((amount,), jnp.int32).at[order[jnp.where(places < fixed, places, moved)]].set(jnp.asarray(lengths, jnp.int32))

    lengths = jnp.where(number % 4 == 0, named(crowded, number // 4), named(usual, number - number // 4 - 1))
    mixed = jax.random.permutation(jax.random.fold_in(own, 3), amount)
    source_of, receiver = mixed[0:amount // 2 * 2:2], mixed[1:amount // 2 * 2:2]
    room = jnp.minimum(lengths[source_of] - 1, bound - lengths[receiver]) // 2
    room = jnp.where((source_of == order[0]) | (receiver == order[0]) | (lengths[receiver] == 0), 0, jnp.maximum(room, 0))
    moved = jax.random.randint(jax.random.fold_in(own, 4), (amount // 2,), 0, 1 << 20) % (room + 1)
    lengths = lengths.at[source_of].add(-moved).at[receiver].add(moved)
    members = jnp.searchsorted(jnp.cumsum(lengths), jnp.arange(rows * top), side="right").astype(jnp.int32)
    table = members.reshape(top, rows).T
    table = table[jax.random.permutation(jax.random.fold_in(own, 1), rows)]
    turn = jax.random.randint(jax.random.fold_in(own, 2), (rows, 1), 0, top)
    return jnp.take_along_axis(table, (jnp.arange(top)[None, :] + turn) % top, axis=1)


def load_shares(count, total, bound, lean, full):
    portions = [(1 << 20) // math.isqrt(standing ** lean) + 1 for standing in range(1, count + 1)]
    largest = bound if full else min(bound, max(-(-total // count), total * portions[0] // sum(portions)))
    least = 1 if total - largest >= count - 1 else 0
    given, rest = [largest] + [least] * (count - 1), total - largest - least * (count - 1)
    while rest > 0:
        free = [i for i in range(1, count) if given[i] < largest] or [i for i in range(1, count) if given[i] < bound]
        whole, budget = sum([portions[i] for i in free]), rest
        for i in free:
            addition = min(bound - given[i], max(1, budget * portions[i] // whole), rest)
            given[i] = given[i] + addition
            rest = rest - addition
    return np.array(given)


def gaussian(stream_key, shape, width, most, split=(), held_as=jnp.bfloat16):
    array = width * jax.random.normal(stream_key, shape, jnp.float32)
    if split:
        array = array * levels(stream_key, shape, split, -0.22, 0.18)
    return jnp.clip(array, -most, most).astype(held_as)


def setup_inputs(seed: int = 0) -> dict:
    key_of = jax.random.split(jax.random.key(seed), 12)
    conv_value = draw_conv_value(jax.random.fold_in(key_of[11], 71), 0)
    conv_gate = gaussian(key_of[1], (TOKENS, CH), 1.5, 8.0, ((0, 8), (1, 4)))
    conv_taps = gaussian(key_of[2], (KW, CH), KW ** -0.5, 1.0, ((1, 4),))
    conv_gain = jnp.clip(1.0 + 0.18 * jax.random.normal(key_of[3], (CH,), jnp.float32), 0.1, 1.9)
    out_weight = gaussian(key_of[4], (CH, D), CH ** -0.5, 0.1875, ((0, 4),))
    residual = gaussian(key_of[5], (TOKENS, D), 1.0, 6.0, ((0, 8),))
    route_ids_keys = jax.random.split(jax.random.fold_in(key_of[6], 1), TOKENS // TOK_DEV)
    route_ids_turns = jax.random.permutation(jax.random.fold_in(key_of[6], 3), TOKENS // TOK_DEV)
    route_ids = jax.vmap(lambda own, number: routed_block(jax.random.fold_in(key_of[6], 2), own, number, TOK_DEV, EXPERTS, TOP_K, CAP, 2))(route_ids_keys, route_ids_turns).reshape((TOKENS, TOP_K))
    route_weight = jnp.clip(jnp.exp(math.log(1.5) - 1.60943787 * jax.random.uniform(key_of[7], (TOKENS, TOP_K), jnp.float32) ** levels(key_of[7], (TOKENS, TOP_K), ((0, 8),), -0.2, 0.2)), 0.3, 1.5)
    expert_gate = gaussian(key_of[8], (EXPERTS, D, EXPERT_FF), D ** -0.5, 0.125, ((0, 8), (2, 4)))
    expert_up = gaussian(key_of[9], (EXPERTS, D, EXPERT_FF), D ** -0.5, 0.125, ((0, 8), (2, 4)))
    expert_down = gaussian(key_of[10], (EXPERTS, EXPERT_FF, D), EXPERT_FF ** -0.5, 0.09375, ((0, 8), (1, 4)))
    return {"conv_value": conv_value, "conv_gate": conv_gate, "conv_taps": conv_taps, "conv_gain": conv_gain, "out_weight": out_weight, "residual": residual, "route_ids": route_ids, "route_weight": route_weight, "expert_gate": expert_gate, "expert_up": expert_up, "expert_down": expert_down}


def slot_plan(block_ids, experts, capacity):
    assigned = block_ids.reshape(-1)
    pair_count = assigned.shape[0]
    onehot = (assigned[:, None] == jnp.arange(experts, dtype=jnp.int32)[None, :]).astype(jnp.int32)
    earlier = jnp.cumsum(onehot, axis=0) - onehot
    ranking = lax.optimization_barrier(jnp.sum(earlier * onehot, axis=1))
    target = assigned * capacity + ranking
    owners = jnp.arange(pair_count, dtype=jnp.int32) // block_ids.shape[1]
    matches = target[None, :] == jnp.arange(experts * capacity, dtype=jnp.int32)[:, None]
    holder = lax.optimization_barrier(jnp.sum(jnp.where(matches, owners[None, :] + 1, 0), axis=1)) - 1
    holder = jnp.where(holder < 0, block_ids.shape[0], holder)
    return (target.astype(jnp.int32), holder.astype(jnp.int32))

def reference(conv_value, conv_gate, conv_taps, conv_gain, out_weight, residual, route_ids, route_weight, expert_gate, expert_up, expert_down):
    gated = conv_value.astype(jnp.float32) * jax.nn.sigmoid(conv_gate.astype(jnp.float32))
    padded = jnp.pad(gated, ((KW - 1, 0), (0, 0)))
    filtered = jnp.zeros((TOKENS, CH), jnp.float32)
    for offset in range(KW):
        filtered = filtered + conv_taps[offset].astype(jnp.float32) * padded[offset:offset + TOKENS]
    average = lax.optimization_barrier(jnp.mean(filtered, axis=1, keepdims=True))
    variance = lax.optimization_barrier(jnp.mean(filtered * filtered, axis=1, keepdims=True)) - average * average
    normed = (filtered - average) * lax.rsqrt(variance + 1e-05) * conv_gain.astype(jnp.float32)
    activated = jax.nn.silu(normed).astype(jnp.bfloat16)
    group_width = CH // N_TP
    mixed = jnp.zeros((TOKENS, D), jnp.float32)
    for group in range(N_TP):
        product = jnp.dot(activated[:, group * group_width:(group + 1) * group_width], out_weight[group * group_width:(group + 1) * group_width], preferred_element_type=jnp.float32)
        mixed = mixed + lax.optimization_barrier(product.astype(jnp.bfloat16)).astype(jnp.float32)
    updated = residual.astype(jnp.float32) + mixed
    normal_rows = (updated * lax.rsqrt(lax.optimization_barrier(jnp.mean(updated * updated, axis=1, keepdims=True)) + 1e-06)).astype(jnp.bfloat16)
    row_blocks = normal_rows.reshape(N_SP, TOK_DEV, D)
    id_blocks = route_ids.reshape(N_SP, TOK_DEV, TOP_K)
    targets, holders = jax.vmap(partial(slot_plan, experts=EXPERTS, capacity=CAP))(id_blocks)
    padded_rows = jnp.concatenate([row_blocks, jnp.zeros((N_SP, 1, D), jnp.bfloat16)], axis=1)
    expert_in = jnp.take_along_axis(padded_rows, holders[:, :, None], axis=1)
    expert_in = jnp.moveaxis(expert_in.reshape(N_SP, EXPERTS, CAP, D), 1, 0).reshape(EXPERTS, N_SP * CAP, D)
    hidden_group = EXPERT_FF // N_TP

    def one_expert(packed):
        rows_in, w_gate, w_up, w_down = packed
        gate_act = jnp.dot(rows_in, w_gate, preferred_element_type=jnp.float32)
        up_act = jnp.dot(rows_in, w_up, preferred_element_type=jnp.float32)
        hidden = (jax.nn.silu(gate_act) * up_act).astype(jnp.bfloat16)
        split_hidden = hidden.reshape(-1, N_TP, hidden_group).astype(jnp.float32)
        split_down = w_down.reshape(N_TP, hidden_group, D).astype(jnp.float32)
        pieces = jnp.einsum('rgf,gfd->grd', split_hidden, split_down)
        pieces = lax.optimization_barrier(pieces.astype(jnp.bfloat16)).astype(jnp.float32)
        return lax.optimization_barrier(jnp.sum(pieces, axis=0)).astype(jnp.bfloat16)
    expert_out = lax.map(one_expert, (expert_in, expert_gate, expert_up, expert_down))
    returned = jnp.moveaxis(expert_out.reshape(EXPERTS, N_SP, CAP, D), 1, 0).reshape(N_SP, EXPERTS * CAP, D)
    picked = jnp.take_along_axis(returned, targets[:, :, None], axis=1).reshape(TOKENS, TOP_K, D)
    combined = lax.optimization_barrier(jnp.sum(picked.astype(jnp.float32) * route_weight[:, :, None], axis=1))
    return (updated + combined).astype(jnp.bfloat16)
```

```python
import functools

import jax
import jax.numpy as jnp
from jax import lax
from jax.experimental import pallas as pl
from jax.experimental.pallas import tpu as pltpu
from jax.sharding import PartitionSpec as P

MESH = pl.DeviceIdType.MESH
F32 = jnp.float32
BF16 = jnp.bfloat16


def passed_along(value, axis, steps):
    count = lax.axis_size(axis)
    initial, last = (max(0, -steps), min(count, count - steps))
    return lax.ppermute(value, axis, [(source, source + steps) for source in range(initial, last)])


def partner(me, d, n):
    if n & (n - 1):
        raise ValueError("sp size")
    out, w = me, 1
    while w < n:
        if d & w:
            out = out + w * (1 - 2 * lax.rem(lax.div(me, w), 2))
        w *= 2
    return out


def ffn_kernel(
    n_sp, n_tp, cap, order, group,
    send, tgt, rw, own, wg_hbm, wu_hbm, wd_hbm, out,
    wg, wu, wd, X, xs, hid, pown, pcs, pcr, q, pys, pyr, eo, back,
    w_sem, l_sem, a_s, a_r, c_s, c_r, y_s, y_r, f_s, f_r, pc_s, pc_r, py_s, py_r, b_s, b_r,
):
    Y = n_tp // 2
    S = n_sp // group
    C = send.shape[1]
    R = cap * group
    me = lax.axis_index("sp")
    t = lax.axis_index("tp")
    y = lax.div(t, 2)
    c = lax.rem(t, 2)
    core = t + 1 - 2 * c

    def ypeer(k):
        return lax.rem(y + k, Y) * 2 + c

    loads = [
        pltpu.make_async_copy(src, dst, w_sem.at[i])
        for i, (src, dst) in enumerate(((wg_hbm, wg), (wu_hbm, wu), (wd_hbm, wd)))
    ]
    for cp in loads:
        cp.start()

    barrier = pltpu.get_barrier_semaphore()
    for d in range(1, n_sp):
        pl.semaphore_signal(barrier, inc=1, device_id=(partner(me, d, n_sp), t), device_id_type=MESH)
    pl.semaphore_signal(barrier, inc=1, device_id=(me, core), device_id_type=MESH)
    for k in range(1, Y):
        pl.semaphore_signal(barrier, inc=1, device_id=(me, ypeer(k)), device_id_type=MESH)
    pl.semaphore_wait(barrier, n_sp - 1 + 1 + Y - 1)

    def remote(src, dst, s_sem, r_sem, dev):
        cp = pltpu.make_async_remote_copy(
            src_ref=src, dst_ref=dst, send_sem=s_sem, recv_sem=r_sem, device_id=dev, device_id_type=MESH
        )
        cp.start()
        return cp

    sent = []
    arrive = {}
    for p, d in enumerate(order):
        dst = partner(me, d, n_sp)
        src = send.at[pl.ds(pl.multiple_of(dst * cap, cap), cap)]
        to = X.at[t, pl.ds(p * cap, cap)]
        if d == 0:
            cp = pltpu.make_async_copy(src, to, l_sem.at[0])
            cp.start()
            arrive[p] = cp
        else:
            cp = remote(src, to, a_s.at[p], a_r.at[p], (dst, t))
            sent.append(cp)
            arrive[p] = cp

    ag_c, ag_y, ag_f, rs_c, rs_y, ret = {}, {}, {}, {}, {}, {}

    def rows(s):
        return pl.ds(s * R, R)

    def stage_a(s):
        for p in range(s * group, (s + 1) * group):
            if order[p] == 0:
                arrive[p].wait()
            else:
                arrive[p].wait_recv()
        mine = X.at[t, rows(s)]
        for k in range(1, Y):
            i = s * Y + k
            ag_y[s, k] = remote(mine, mine, y_s.at[i], y_r.at[i], (me, ypeer(k)))
        ag_c[s] = remote(mine, mine, c_s.at[s], c_r.at[s], (me, core))

    def stage_b(s):
        for k in range(1, Y):
            ag_y[s, k].wait_recv()
            i = s * Y + k
            got = X.at[lax.rem(y + Y - k, Y) * 2 + c, rows(s)]
            ag_f[s, k] = remote(got, got, f_s.at[i], f_r.at[i], (me, core))

    tile = 256

    def stage_c(s):
        ag_c[s].wait_recv()
        for k in range(1, Y):
            ag_f[s, k].wait_recv()
        for j in range(n_tp):
            xs[:, j * C:(j + 1) * C] = X[j, rows(s), :]
        if s == 0:
            for cp in loads:
                cp.wait()

        def up(n, carry):
            cols = pl.ds(pl.multiple_of(n * tile, tile), tile)
            x = xs[...]
            g = jnp.dot(x, wg[:, cols], preferred_element_type=F32)
            u = jnp.dot(x, wu[:, cols], preferred_element_type=F32)
            hid[:, cols] = (g / (1.0 + jnp.exp(-g)) * u).astype(BF16)
            return carry

        lax.fori_loop(0, hid.shape[1] // tile, up, 0)

        def theirs(yy, carry):
            cols = pl.ds(pl.multiple_of((yy * 2 + 1 - c) * C, C), C)
            pcs[s, yy] = jnp.dot(hid[...], wd[:, cols], preferred_element_type=F32).astype(BF16)
            return carry

        lax.fori_loop(0, Y, theirs, 0)
        rs_c[s] = remote(pcs.at[s], pcr.at[s], pc_s.at[s], pc_r.at[s], (me, core))

        def ours(yy, carry):
            cols = pl.ds(pl.multiple_of((yy * 2 + c) * C, C), C)
            pown[yy] = jnp.dot(hid[...], wd[:, cols], preferred_element_type=F32)
            return carry

        lax.fori_loop(0, Y, ours, 0)

    def stage_d(s):
        rs_c[s].wait_recv()
        for k in range(1, Y):
            yy = lax.rem(y + k, Y)
            i = s * Y + k
            pys[i] = (pown[yy] + pcr[s, yy].astype(F32)).astype(BF16)
            rs_y[s, k] = remote(pys.at[i], pyr.at[i], py_s.at[i], py_r.at[i], (me, ypeer(k)))
        q[s] = pown[y] + pcr[s, y].astype(F32)

    def stage_e(s):
        total = q[s]
        for k in range(1, Y):
            rs_y[s, k].wait_recv()
            total = total + pyr[s * Y + k].astype(F32)
        eo[rows(s)] = total.astype(BF16)
        for p in range(s * group, (s + 1) * group):
            d = order[p]
            dst = partner(me, d, n_sp)
            src = eo.at[pl.ds(p * cap, cap)]
            to = back.at[pl.ds(pl.multiple_of(me * cap, cap), cap)]
            if d == 0:
                cp = pltpu.make_async_copy(src, to, l_sem.at[1])
                cp.start()
            else:
                cp = remote(src, to, b_s.at[p], b_r.at[p], (dst, t))
            ret[p] = cp

    stage_a(0)
    stage_b(0)
    for s in range(S):
        if s + 1 < S:
            stage_a(s + 1)
        stage_c(s)
        if s + 1 < S:
            stage_b(s + 1)
        stage_d(s)
        if s > 0:
            stage_e(s - 1)
    stage_e(S - 1)

    for p, d in enumerate(order):
        if d == 0:
            ret[p].wait()
        else:
            ret[p].wait_recv()
    total = own[...]
    places = lax.broadcasted_iota(jnp.int32, (total.shape[0], back.shape[0]), 1)
    for k in range(tgt.shape[1]):
        pick = jnp.where(places == tgt[:, k:k + 1], 1.0, 0.0).astype(BF16)
        total = total + rw[:, k:k + 1] * jnp.dot(pick, back[...], preferred_element_type=F32)
    out[...] = total.astype(BF16)

    for cp in sent:
        cp.wait_send()
    for table in (ag_c, ag_y, ag_f, rs_c, rs_y):
        for cp in table.values():
            cp.wait_send()
    for p, d in enumerate(order):
        if d != 0:
            ret[p].wait_send()


def routed_ffn(send, targets, route_weight, own, w_gate, w_up, w_down, cap):
    n_sp, n_tp = lax.axis_size("sp"), lax.axis_size("tp")
    group = max(1, min(n_sp, 256 // cap))
    order = list(range(n_sp))
    if n_sp == 8:
        order = [0, 1, 4, 5, 6, 7, 2, 3]
    S, Y, C, R = n_sp // group, n_tp // 2, send.shape[1], cap * group
    width, hidden = w_gate.shape
    tokens = own.shape[0]
    dma = pltpu.SemaphoreType.DMA
    vm = pl.BlockSpec(memory_space=pltpu.VMEM)
    hb = pl.BlockSpec(memory_space=pl.ANY)
    return pl.pallas_call(
        functools.partial(ffn_kernel, n_sp, n_tp, cap, order, group),
        out_shape=jax.ShapeDtypeStruct((tokens, C), BF16),
        in_specs=[vm, vm, vm, vm, hb, hb, hb],
        out_specs=vm,
        scratch_shapes=[
            pltpu.VMEM((width, hidden), BF16),
            pltpu.VMEM((width, hidden), BF16),
            pltpu.VMEM((hidden, width), BF16),
            pltpu.VMEM((n_tp, n_sp * cap, C), BF16),
            pltpu.VMEM((R, width), BF16),
            pltpu.VMEM((R, hidden), BF16),
            pltpu.VMEM((Y, R, C), F32),
            pltpu.VMEM((S, Y, R, C), BF16),
            pltpu.VMEM((S, Y, R, C), BF16),
            pltpu.VMEM((S, R, C), F32),
            pltpu.VMEM((S * Y, R, C), BF16),
            pltpu.VMEM((S * Y, R, C), BF16),
            pltpu.VMEM((n_sp * cap, C), BF16),
            pltpu.VMEM((n_sp * cap, C), BF16),
            dma((3,)), dma((2,)),
            dma((n_sp,)), dma((n_sp,)),
            dma((S,)), dma((S,)),
            dma((S * Y,)), dma((S * Y,)),
            dma((S * Y,)), dma((S * Y,)),
            dma((S,)), dma((S,)),
            dma((S * Y,)), dma((S * Y,)),
            dma((n_sp,)), dma((n_sp,)),
        ],
        compiler_params=pltpu.CompilerParams(
            collective_id=1, has_side_effects=True, vmem_limit_bytes=60 * 1024 * 1024
        ),
    )(send, targets, route_weight, own, w_gate, w_up, w_down)


def slot_targets(block_ids, experts, capacity):
    assigned = block_ids.reshape(-1)
    onehot = (assigned[:, None] == jnp.arange(experts, dtype=jnp.int32)[None, :]).astype(jnp.int32)
    earlier = jnp.cumsum(onehot, axis=0) - onehot
    ranking = jnp.sum(earlier * onehot, axis=1)
    return (assigned * capacity + ranking).reshape(block_ids.shape)


def local(
    conv_value,
    conv_gate,
    conv_taps,
    conv_gain,
    out_weight,
    residual,
    route_ids,
    route_weight,
    expert_gate,
    expert_up,
    expert_down,
):
    taps_count = conv_taps.shape[0]
    token_rows = conv_value.shape[0]
    experts = lax.axis_size("sp")
    top_count = route_ids.shape[1]
    capacity = 2 * token_rows * top_count // experts
    targets = slot_targets(route_ids, experts, capacity)
    tails = passed_along(
        jnp.concatenate(
            [conv_value[token_rows - taps_count + 1:], conv_gate[token_rows - taps_count + 1:]], axis=1
        ),
        "sp",
        1,
    )
    chans = conv_value.shape[1]
    values_ext = jnp.concatenate([tails[:, :chans], conv_value], axis=0)
    gates_ext = jnp.concatenate([tails[:, chans:], conv_gate], axis=0)
    gated = values_ext.astype(F32) * jax.nn.sigmoid(gates_ext.astype(F32))
    filtered = jnp.zeros(conv_value.shape, F32)
    for offset in range(taps_count):
        filtered = filtered + conv_taps[offset].astype(F32) * gated[offset:offset + token_rows]
    channels = chans * lax.axis_size("tp")
    totals = lax.psum((jnp.sum(filtered, axis=1), jnp.sum(filtered * filtered, axis=1)), "tp")
    average = totals[0] / channels
    variance = totals[1] / channels - average * average
    normed = (filtered - average[:, None]) * lax.rsqrt(variance + 1e-05)[:, None] * conv_gain
    activated = jax.nn.silu(normed).astype(BF16)
    mixed = lax.psum_scatter(
        jnp.dot(activated, out_weight, preferred_element_type=F32).astype(BF16),
        "tp", scatter_dimension=1, tiled=True,
    ).astype(F32)
    width = residual.shape[1]
    columns = mixed.shape[1]
    own = lax.dynamic_slice_in_dim(residual, lax.axis_index("tp") * columns, columns, 1).astype(F32) + mixed
    squares = lax.psum(jnp.sum(own * own, axis=1, keepdims=True), "tp") / width
    normal = (own * lax.rsqrt(squares + 1e-06)).astype(BF16)
    slots = jnp.arange(experts * capacity, dtype=jnp.int32)
    pick = functools.reduce(
        jnp.logical_or, [slots[:, None] == targets[None, :, k] for k in range(top_count)]
    ).astype(BF16)
    send = jnp.dot(pick, normal, preferred_element_type=F32).astype(BF16)
    return routed_ffn(
        send, targets, route_weight, own, expert_gate[0], expert_up[0], expert_down[0], capacity
    )


def solution(mesh):
    placed = (
        P("sp", "tp"),
        P("sp", "tp"),
        P(None, "tp"),
        P("tp"),
        P("tp", None),
        P("sp", None),
        P("sp", None),
        P("sp", None),
        P("sp", None, "tp"),
        P("sp", None, "tp"),
        P("sp", "tp", None),
    )
    return jax.shard_map(
        local, mesh=mesh, in_specs=placed, out_specs=P("sp", "tp"), check_vma=False
    )
```

```python
import functools

import jax
import jax.numpy as jnp
from jax import lax
from jax.experimental import pallas as pl
from jax.experimental.pallas import tpu as pltpu
from jax.sharding import PartitionSpec as P

MESH = pl.DeviceIdType.MESH
F32 = jnp.float32
BF16 = jnp.bfloat16


def partner(me, d, n):
    if n & (n - 1):
        raise ValueError("sp size")
    out, w = me, 1
    while w < n:
        if d & w:
            out = out + w * (1 - 2 * lax.rem(lax.div(me, w), 2))
        w *= 2
    return out


def as_row(first, second):
    lanes = lax.broadcasted_iota(jnp.int32, (first.shape[0], 128), 1)
    both = jnp.where(lanes == 0, first, jnp.where(lanes == 1, second, 0.0))
    return both.T[0:8]


def as_columns(rows8):
    return jnp.concatenate([rows8] * 16, axis=0).T


def stacked(rows):
    place = lax.broadcasted_iota(jnp.int32, (8, rows[0].shape[1]), 0)
    out = jnp.zeros((8, rows[0].shape[1]), F32)
    for i, r in enumerate(rows):
        out = jnp.where(place == i, r, out)
    return out


def layer_kernel(
    n_sp, n_tp, cap, order, group, halo_rows,
    value, gate, taps, gain, ids, rwt, ow_hbm, res_hbm, wg_hbm, wu_hbm, wd_hbm, out,
    ow, res, halo, G, fil, st_s, st_r, act, p1s, p1r, p1own, y1s, y1r, own, nrm, pickt, meta, send,
    wg, wu, wd, X, xs, hid, pown, pcs, pcr, q, pys, pyr, eo, back,
    o_sem, h_s, h_r, s_s, s_r, p1_s, p1_r, y1_s, y1_r,
    w_sem, l_sem, a_s, a_r, c_s, c_r, y_s, y_r, f_s, f_r, pc_s, pc_r, py_s, py_r, b_s, b_r,
):
    Y = n_tp // 2
    S = n_sp // group
    C = send.shape[1]
    R = cap * group
    T, chans = value.shape
    taps_count = taps.shape[0]
    top = ids.shape[0]
    me = lax.axis_index("sp")
    t = lax.axis_index("tp")
    y = lax.div(t, 2)
    c = lax.rem(t, 2)
    core = t + 1 - 2 * c

    def ypeer(k):
        return lax.rem(y + k, Y) * 2 + c

    barrier = pltpu.get_barrier_semaphore()
    for d in range(1, n_sp):
        pl.semaphore_signal(barrier, inc=1, device_id=(partner(me, d, n_sp), t), device_id_type=MESH)
    for j in range(1, n_tp):
        pl.semaphore_signal(barrier, inc=1, device_id=(me, lax.rem(t + j, n_tp)), device_id_type=MESH)

    cols_own = pl.ds(pl.multiple_of(t * C, C), C)
    early = [
        pltpu.make_async_copy(ow_hbm, ow, o_sem.at[0]),
        pltpu.make_async_copy(res_hbm.at[:, cols_own], res, o_sem.at[1]),
    ]
    loads = [
        pltpu.make_async_copy(src, dst, w_sem.at[i])
        for i, (src, dst) in enumerate(((wg_hbm, wg), (wu_hbm, wu), (wd_hbm, wd)))
    ]
    for cp in early + loads:
        cp.start()

    def gated(v, g):
        g = g.astype(F32)
        return v.astype(F32) / (1.0 + jnp.exp(-g))

    H = halo_rows
    G[H:H + T, :] = gated(value[...], gate[...])

    pl.semaphore_wait(barrier, n_sp - 1 + n_tp - 1)

    def remote(src, dst, s_sem, r_sem, dev, start=True):
        cp = pltpu.make_async_remote_copy(
            src_ref=src, dst_ref=dst, send_sem=s_sem, recv_sem=r_sem, device_id=dev, device_id_type=MESH
        )
        if start:
            cp.start()
        return cp

    after = lax.rem(me + 1, n_sp)
    tails = [
        remote(x.at[pl.ds(T - H, H)], halo.at[i], h_s.at[i], h_r.at[i], (after, t), start=False)
        for i, x in enumerate((value, gate))
    ]

    @pl.when(me < n_sp - 1)
    def _():
        for cp in tails:
            cp.start()

    row_ids = ids[...].astype(F32)
    experts = lax.broadcasted_iota(jnp.int32, (n_sp, T), 0).astype(F32)
    hot = [jnp.where(experts == row_ids[k:k + 1, :], 1.0, 0.0) for k in range(top)]
    counts = functools.reduce(jnp.add, hot)
    before = lax.broadcasted_iota(jnp.int32, (T, T), 0) < lax.broadcasted_iota(jnp.int32, (T, T), 1)
    earlier = jnp.dot(
        counts.astype(BF16), jnp.where(before, 1.0, 0.0).astype(BF16), preferred_element_type=F32
    )
    target = [
        row_ids[k:k + 1, :] * cap + jnp.sum(hot[k] * earlier, axis=0, keepdims=True) for k in range(top)
    ]
    slots = lax.broadcasted_iota(jnp.int32, (n_sp * cap, T), 0).astype(F32)
    pickt[...] = functools.reduce(
        jnp.add, [jnp.where(slots == target[k], 1.0, 0.0) for k in range(top)]
    ).astype(BF16)
    meta[...] = as_columns(stacked(target + [rwt[k:k + 1, :] for k in range(top)]))

    step_rows, step_lanes = 64, min(128, chans)
    taps32 = taps[...].astype(F32)

    def filter_rows(r):
        for l in range(0, chans, step_lanes):
            total = jnp.zeros((step_rows, step_lanes), F32)
            for i in range(taps_count):
                at = H - taps_count + 1 + r + i
                total = total + taps32[i:i + 1, l:l + step_lanes] * G[at:at + step_rows, l:l + step_lanes]
            fil[r:r + step_rows, l:l + step_lanes] = total

    for r in range(step_rows, T, step_rows):
        filter_rows(r)

    @pl.when(me > 0)
    def _():
        for cp in tails:
            cp.wait_recv()
        G[0:H, :] = gated(halo[0], halo[1])

    @pl.when(me == 0)
    def _():
        G[0:H, :] = jnp.zeros((H, chans), F32)

    filter_rows(0)

    sent = []

    def over_tp(which, rows8):
        st_s[which] = rows8
        cps = []
        for j in range(1, n_tp):
            i = which * n_tp + j
            cps.append(
                remote(st_s.at[which], st_r.at[i], s_s.at[i], s_r.at[i], (me, lax.rem(t + j, n_tp)))
            )
        total = rows8
        for j, cp in enumerate(cps):
            cp.wait_recv()
            total = total + st_r[which * n_tp + j + 1]
        sent.extend(cps)
        return total

    f = fil[...]
    sums = over_tp(0, as_row(jnp.sum(f, axis=1, keepdims=True), jnp.sum(f * f, axis=1, keepdims=True)))
    channels = chans * n_tp
    average = sums[0:1] / channels
    variance = sums[1:2] / channels - average * average
    cols = as_columns(stacked([average, lax.rsqrt(variance + 1e-05)]))
    normed = (fil[...] - cols[:, 0:1]) * cols[:, 1:2] * gain[...]
    act[...] = (normed / (1.0 + jnp.exp(-normed))).astype(BF16)
    for cp in early:
        cp.wait()

    p1 = {}
    for k in list(range(1, Y)) + [0]:
        yy = lax.rem(y + k, Y)
        at = pl.ds(pl.multiple_of((yy * 2 + 1 - c) * C, C), C)
        p1s[k] = jnp.dot(act[...], ow[:, at], preferred_element_type=F32).astype(BF16)
        p1[k] = remote(p1s.at[k], p1r.at[k], p1_s.at[k], p1_r.at[k], (me, core))
    for k in list(range(1, Y)) + [0]:
        yy = lax.rem(y + k, Y)
        at = pl.ds(pl.multiple_of((yy * 2 + c) * C, C), C)
        p1own[k] = jnp.dot(act[...], ow[:, at], preferred_element_type=F32)
    y1 = {}
    for k in range(1, Y):
        p1[k].wait_recv()
        y1s[k] = (p1own[k] + p1r[k].astype(F32)).astype(BF16)
        y1[k] = remote(y1s.at[k], y1r.at[k], y1_s.at[k], y1_r.at[k], (me, ypeer(k)))
    p1[0].wait_recv()
    stream = res[...].astype(F32) + p1own[0] + p1r[0].astype(F32)
    for k in range(1, Y):
        y1[k].wait_recv()
        stream = stream + y1r[k].astype(F32)
    own[...] = stream
    sent.extend(p1.values())
    sent.extend(y1.values())
    square = jnp.sum(stream * stream, axis=1, keepdims=True)
    squares = over_tp(1, as_row(square, jnp.zeros_like(square)))
    scale = as_columns(stacked([lax.rsqrt(squares[0:1] / (C * n_tp) + 1e-06)]))[:, 0:1]
    nrm[...] = (own[...] * scale).astype(BF16)

    arrive = {}
    for p, d in enumerate(order):
        dst = partner(me, d, n_sp)
        at = pl.ds(pl.multiple_of(dst * cap, cap), cap)
        block = jnp.dot(pickt[at, :], nrm[...], preferred_element_type=F32).astype(BF16)
        if d == 0:
            X[t, p * cap:(p + 1) * cap, :] = block
        else:
            mine = pl.ds(p * cap, cap)
            send[mine, :] = block
            cp = remote(send.at[mine], X.at[t, mine], a_s.at[p], a_r.at[p], (dst, t))
            sent.append(cp)
            arrive[p] = cp

    ag_c, ag_y, ag_f, rs_c, rs_y, ret = {}, {}, {}, {}, {}, {}

    def rows(s):
        return pl.ds(s * R, R)

    def stage_a(s):
        for p in range(s * group, (s + 1) * group):
            if order[p] != 0:
                arrive[p].wait_recv()
        mine = X.at[t, rows(s)]
        for k in range(1, Y):
            i = s * Y + k
            ag_y[s, k] = remote(mine, mine, y_s.at[i], y_r.at[i], (me, ypeer(k)))
        ag_c[s] = remote(mine, mine, c_s.at[s], c_r.at[s], (me, core))

    def stage_b(s):
        for k in range(1, Y):
            ag_y[s, k].wait_recv()
            i = s * Y + k
            got = X.at[lax.rem(y + Y - k, Y) * 2 + c, rows(s)]
            ag_f[s, k] = remote(got, got, f_s.at[i], f_r.at[i], (me, core))

    tile = 256

    def stage_c(s):
        ag_c[s].wait_recv()
        for k in range(1, Y):
            ag_f[s, k].wait_recv()
        for j in range(n_tp):
            xs[:, j * C:(j + 1) * C] = X[j, rows(s), :]
        if s == 0:
            for cp in loads:
                cp.wait()

        def up(n, carry):
            cols = pl.ds(pl.multiple_of(n * tile, tile), tile)
            x = xs[...]
            g = jnp.dot(x, wg[:, cols], preferred_element_type=F32)
            u = jnp.dot(x, wu[:, cols], preferred_element_type=F32)
            hid[:, cols] = (g / (1.0 + jnp.exp(-g)) * u).astype(BF16)
            return carry

        lax.fori_loop(0, hid.shape[1] // tile, up, 0)

        def theirs(yy, carry):
            cols = pl.ds(pl.multiple_of((yy * 2 + 1 - c) * C, C), C)
            pcs[s, yy] = jnp.dot(hid[...], wd[:, cols], preferred_element_type=F32).astype(BF16)
            return carry

        lax.fori_loop(0, Y, theirs, 0)
        rs_c[s] = remote(pcs.at[s], pcr.at[s], pc_s.at[s], pc_r.at[s], (me, core))

        def ours(yy, carry):
            cols = pl.ds(pl.multiple_of((yy * 2 + c) * C, C), C)
            pown[yy] = jnp.dot(hid[...], wd[:, cols], preferred_element_type=F32)
            return carry

        lax.fori_loop(0, Y, ours, 0)

    def stage_d(s):
        rs_c[s].wait_recv()
        for k in range(1, Y):
            yy = lax.rem(y + k, Y)
            i = s * Y + k
            pys[i] = (pown[yy] + pcr[s, yy].astype(F32)).astype(BF16)
            rs_y[s, k] = remote(pys.at[i], pyr.at[i], py_s.at[i], py_r.at[i], (me, ypeer(k)))
        q[s] = pown[y] + pcr[s, y].astype(F32)

    def stage_e(s):
        total = q[s]
        for k in range(1, Y):
            rs_y[s, k].wait_recv()
            total = total + pyr[s * Y + k].astype(F32)
        eo[rows(s)] = total.astype(BF16)
        for p in range(s * group, (s + 1) * group):
            d = order[p]
            dst = partner(me, d, n_sp)
            src = eo.at[pl.ds(p * cap, cap)]
            to = back.at[pl.ds(pl.multiple_of(me * cap, cap), cap)]
            if d == 0:
                cp = pltpu.make_async_copy(src, to, l_sem.at[1])
                cp.start()
            else:
                cp = remote(src, to, b_s.at[p], b_r.at[p], (dst, t))
            ret[p] = cp

    stage_a(0)
    stage_b(0)
    for s in range(S):
        if s + 1 < S:
            stage_a(s + 1)
        stage_c(s)
        if s + 1 < S:
            stage_b(s + 1)
        stage_d(s)
        if s > 0:
            stage_e(s - 1)
    stage_e(S - 1)

    for p, d in enumerate(order):
        if d == 0:
            ret[p].wait()
        else:
            ret[p].wait_recv()
    total = own[...]
    places = lax.broadcasted_iota(jnp.int32, (total.shape[0], back.shape[0]), 1).astype(F32)
    for k in range(top):
        pick = jnp.where(places == meta[:, k:k + 1], 1.0, 0.0).astype(BF16)
        total = total + meta[:, top + k:top + k + 1] * jnp.dot(pick, back[...], preferred_element_type=F32)
    out[...] = total.astype(BF16)

    @pl.when(me < n_sp - 1)
    def _():
        for cp in tails:
            cp.wait_send()

    for cp in sent:
        cp.wait_send()
    for table in (ag_c, ag_y, ag_f, rs_c, rs_y):
        for cp in table.values():
            cp.wait_send()
    for p, d in enumerate(order):
        if d != 0:
            ret[p].wait_send()


def local(
    conv_value,
    conv_gate,
    conv_taps,
    conv_gain,
    out_weight,
    residual,
    route_ids,
    route_weight,
    expert_gate,
    expert_up,
    expert_down,
):
    n_sp, n_tp = lax.axis_size("sp"), lax.axis_size("tp")
    T, chans = conv_value.shape
    top = route_ids.shape[1]
    width, hidden = expert_gate.shape[1:]
    cap = 2 * T * top // n_sp
    C = width // n_tp
    halo_rows = -(-(conv_taps.shape[0] - 1) // 16) * 16
    group = max(1, min(n_sp, 256 // cap))
    order = list(range(n_sp))
    if n_sp == 8:
        order = [0, 1, 4, 5, 6, 7, 2, 3]
    S, Y, R = n_sp // group, n_tp // 2, cap * group
    dma = pltpu.SemaphoreType.DMA
    vm = pl.BlockSpec(memory_space=pltpu.VMEM)
    hb = pl.BlockSpec(memory_space=pl.ANY)
    return pl.pallas_call(
        functools.partial(layer_kernel, n_sp, n_tp, cap, order, group, halo_rows),
        out_shape=jax.ShapeDtypeStruct((T, C), BF16),
        in_specs=[vm] * 6 + [hb] * 5,
        out_specs=vm,
        scratch_shapes=[
            pltpu.VMEM((chans, width), BF16),
            pltpu.VMEM((T, C), BF16),
            pltpu.VMEM((2, halo_rows, chans), BF16),
            pltpu.VMEM((halo_rows + T, chans), F32),
            pltpu.VMEM((T, chans), F32),
            pltpu.VMEM((2, 8, T), F32),
            pltpu.VMEM((2 * n_tp, 8, T), F32),
            pltpu.VMEM((T, chans), BF16),
            pltpu.VMEM((Y, T, C), BF16),
            pltpu.VMEM((Y, T, C), BF16),
            pltpu.VMEM((Y, T, C), F32),
            pltpu.VMEM((Y, T, C), BF16),
            pltpu.VMEM((Y, T, C), BF16),
            pltpu.VMEM((T, C), F32),
            pltpu.VMEM((T, C), BF16),
            pltpu.VMEM((n_sp * cap, T), BF16),
            pltpu.VMEM((T, 128), F32),
            pltpu.VMEM((n_sp * cap, C), BF16),
            pltpu.VMEM((width, hidden), BF16),
            pltpu.VMEM((width, hidden), BF16),
            pltpu.VMEM((hidden, width), BF16),
            pltpu.VMEM((n_tp, n_sp * cap, C), BF16),
            pltpu.VMEM((R, width), BF16),
            pltpu.VMEM((R, hidden), BF16),
            pltpu.VMEM((Y, R, C), F32),
            pltpu.VMEM((S, Y, R, C), BF16),
            pltpu.VMEM((S, Y, R, C), BF16),
            pltpu.VMEM((S, R, C), F32),
            pltpu.VMEM((S * Y, R, C), BF16),
            pltpu.VMEM((S * Y, R, C), BF16),
            pltpu.VMEM((n_sp * cap, C), BF16),
            pltpu.VMEM((n_sp * cap, C), BF16),
            dma((2,)), dma((2,)), dma((2,)),
            dma((2 * n_tp,)), dma((2 * n_tp,)),
            dma((Y,)), dma((Y,)),
            dma((Y,)), dma((Y,)),
            dma((3,)), dma((2,)),
            dma((n_sp,)), dma((n_sp,)),
            dma((S,)), dma((S,)),
            dma((S * Y,)), dma((S * Y,)),
            dma((S * Y,)), dma((S * Y,)),
            dma((S,)), dma((S,)),
            dma((S * Y,)), dma((S * Y,)),
            dma((n_sp,)), dma((n_sp,)),
        ],
        compiler_params=pltpu.CompilerParams(
            collective_id=1, has_side_effects=True, vmem_limit_bytes=60 * 1024 * 1024
        ),
    )(
        conv_value, conv_gate, conv_taps, conv_gain.reshape(1, chans), route_ids.T, route_weight.T,
        out_weight, residual, expert_gate[0], expert_up[0], expert_down[0],
    )


def solution(mesh):
    placed = (
        P("sp", "tp"),
        P("sp", "tp"),
        P(None, "tp"),
        P("tp"),
        P("tp", None),
        P("sp", None),
        P("sp", None),
        P("sp", None),
        P("sp", None, "tp"),
        P("sp", None, "tp"),
        P("sp", "tp", None),
    )
    return jax.shard_map(
        local, mesh=mesh, in_specs=placed, out_specs=P("sp", "tp"), check_vma=False
    )
```
